32 devices in a mesh: sp: 8 (over z, x), tp: 4 (over y, core).
Axes of the slice: x: 2, y: 2, z: 4, core: 2. Of those that a mesh axis runs over, the one named last changes fastest.
Arguments:
- hidden_in: bfloat16 [2048, 2048], P('sp'), may hold values from -8 to 8
- w_convb: bfloat16 [2048, 1024], P('sp', 'tp'), may hold values from -0.125 to 0.125
- w_convc: bfloat16 [2048, 1024], P('sp', 'tp'), may hold values from -0.125 to 0.125
- w_convx: bfloat16 [2048, 1024], P('sp', 'tp'), may hold values from -0.125 to 0.125
- w_query: bfloat16 [2048, 1024], P('sp', 'tp'), may hold values from -1 to 1
- w_key: bfloat16 [2048, 1024], P('sp', 'tp'), may hold values from -1 to 1
- w_value: bfloat16 [2048, 1024], P('sp', 'tp'), may hold values from -0.125 to 0.125
- conv_taps: float32 [3, 1024], P(None, 'tp'), may hold values from -3.5 to 3.5
- gate_cache: float32 [2048, 16], P(None, 'tp'), as said below
- w_out_conv: bfloat16 [1024, 2048], P('tp'), may hold values from -0.125 to 0.125
- w_out_attn: bfloat16 [1024, 2048], P('tp'), may hold values from -0.125 to 0.125
Outputs:
- mixed: bfloat16 [2048, 2048], P(('sp', 'tp'))
The draws below stay inside these ranges and needn't reach their ends.
Inputs may be any that keep to these rules, and one draw needn't show every extreme that they name: `gate_cache`: down each column, read from row 256 to the last row and then from row 0 on, the values never rise.
All inputs are finite; a program needn't handle non-finite values.
Results may differ from the reference program's by a relative error of at most 0.018.
Values may be sent and summed in bfloat16 or wider, within the bound.
A program may use at most 128 MiB of HBM per device.

```python
import math
import jax
import jax.numpy as jnp
from jax import lax

D = 2048
CONV = 1024
HEADS = 16
HD = 64
TOK_DEV = 256
STREAM_EXTENT = 512
ROLL_ROWS = 256
ATTW = 1024
ENTRIES_OVERALL = 2048
N_TP = 4


def weight_pairs(key):
    base = jnp.clip(jax.random.normal(jax.random.fold_in(key, 101), (D, HEADS * HD), jnp.float32), -8.0, 8.0)
    other = jnp.clip(jax.random.normal(jax.random.fold_in(key, 202), (D, HEADS * HD), jnp.float32), -8.0, 8.0)
    keyed = other
    factor = 1.7 * D ** (-0.5)
    return (base * factor, jnp.clip(keyed, -8.0, 8.0) * factor)


def draw_w_query(key, part):
    return weight_pairs(key)[0].astype(jnp.bfloat16)


def draw_w_key(key, part):
    return weight_pairs(key)[1].astype(jnp.bfloat16)


def draw_hidden_in(key, part):
    base = jax.random.normal(jax.random.fold_in(key, 1), (ENTRIES_OVERALL, D), jnp.float32)
    return jnp.clip(base, -8.0, 8.0).astype(jnp.bfloat16)


def draw_gate_cache(key, part):
    order = jax.random.permutation(jax.random.fold_in(key, 11), HEADS)
    slow_count = HEADS // 2
    slow = (order < slow_count).astype(jnp.float32)
    fast_rate = jnp.exp(jax.random.uniform(jax.random.fold_in(key, 12), (HEADS,), jnp.float32, math.log(1.0 / 100.0), math.log(1.0 / 30.0)))
    slow_rate = jax.random.uniform(jax.random.fold_in(key, 13), (HEADS,), jnp.float32, 0.3, 0.8) / STREAM_EXTENT
    rate = slow * slow_rate + (1.0 - slow) * fast_rate
    block_factor = jnp.exp(jax.random.uniform(jax.random.fold_in(key, 14), (ENTRIES_OVERALL // TOK_DEV, 1, HEADS), jnp.float32, math.log(0.5), math.log(2.0)))
    roughness = jax.random.uniform(jax.random.fold_in(key, 15), (ENTRIES_OVERALL // TOK_DEV, TOK_DEV, HEADS), jnp.float32, 0.3, 1.7)
    opening_scores = -(rate * block_factor * roughness).reshape(ENTRIES_OVERALL, HEADS)
    spike_clusters = jax.random.bernoulli(jax.random.fold_in(key, 16), 2.0 / STREAM_EXTENT, (ENTRIES_OVERALL, 1))
    objective_errors = jax.random.uniform(jax.random.fold_in(key, 17), (ENTRIES_OVERALL, HEADS), jnp.float32, math.log(0.5), math.log(0.8))
    opening_scores = opening_scores + jnp.where(spike_clusters, objective_errors, 0.0)
    return jnp.roll(jnp.cumsum(opening_scores, axis=0), ROLL_ROWS, axis=0)


def block_scale(own_key, dims, split, smallest, high):
    def one(axis_at, blocks):
        draws = jax.random.uniform(jax.random.fold_in(jax.random.fold_in(own_key, 6), axis_at), (blocks,), jnp.float32, smallest / len(split), high / len(split))
        return jnp.repeat(jnp.exp(draws), dims[axis_at] // blocks).reshape((-1,) + (1,) * (len(dims) - axis_at - 1))

    loudness = one(*split[0])
    for cut in split[1:]:
        loudness = loudness * one(*cut)
    return loudness


def scatter_about(stream_key, dims, spread, most, split=(), held_as=jnp.bfloat16):
    values = jax.random.normal(stream_key, dims, jnp.float32) * spread
    if len(split) > 0:
        values = block_scale(stream_key, dims, split, -0.22, 0.18) * values
    return jnp.clip(values, min=-most, max=most).astype(held_as)


def setup_inputs(seed: int = 0) -> dict:
    key_of = jax.random.split(jax.random.key(seed), 12)
    hidden_in = draw_hidden_in(jax.random.fold_in(key_of[11], 71), 0)
    w_convb = scatter_about(key_of[1], (D, CONV), D ** -0.5, 0.125, ((0, 8), (1, 4)))
    w_convc = scatter_about(key_of[2], (D, CONV), D ** -0.5, 0.125, ((0, 8), (1, 4)))
    w_convx = scatter_about(key_of[3], (D, CONV), D ** -0.5, 0.125, ((0, 8), (1, 4)))
    w_query = draw_w_query(jax.random.fold_in(key_of[11], 71), 0)
    w_key = draw_w_key(jax.random.fold_in(key_of[11], 71), 0)
    w_value = scatter_about(key_of[6], (D, ATTW), D ** -0.5, 0.125, ((0, 8), (1, 4)))
    conv_taps = scatter_about(key_of[7], (3, CONV), 3 ** -0.5, 3.5, ((1, 4),), jnp.float32)
    gate_cache = draw_gate_cache(jax.random.fold_in(key_of[11], 71), 0)
    w_out_conv = scatter_about(key_of[9], (CONV, D), (CONV + HEADS * HD) ** -0.5, 0.125, ((0, 4),))
    w_out_attn = scatter_about(key_of[10], (ATTW, D), (CONV + HEADS * HD) ** -0.5, 0.125, ((0, 4),))
    return {"hidden_in": hidden_in, "w_convb": w_convb, "w_convc": w_convc, "w_convx": w_convx, "w_query": w_query, "w_key": w_key, "w_value": w_value, "conv_taps": conv_taps, "gate_cache": gate_cache, "w_out_conv": w_out_conv, "w_out_attn": w_out_attn}


neg_large = -1e30


def project(hidden_in, weight):
    return jnp.dot(hidden_in, weight, preferred_element_type=jnp.float32).astype(jnp.bfloat16)


def short_conv(gate_b, gate_c, conv_values, conv_taps):
    conv_input = (gate_c.astype(jnp.float32) * conv_values.astype(jnp.float32)).astype(jnp.bfloat16)
    conv_input = lax.optimization_barrier(conv_input)
    framed = conv_input.reshape(-1, STREAM_EXTENT, CONV).astype(jnp.float32)
    padded = jnp.pad(framed, ((0, 0), (2, 0), (0, 0)))
    mixed_rows = conv_taps[0] * padded[:, :STREAM_EXTENT] + conv_taps[1] * padded[:, 1:STREAM_EXTENT + 1] + conv_taps[2] * padded[:, 2:]
    return (gate_b.astype(jnp.float32) * mixed_rows.reshape(-1, CONV)).astype(jnp.bfloat16)


def attention(query, keys, values, gate_cache):
    seq_count = query.shape[0] // STREAM_EXTENT

    def heads_first(array):
        return array.reshape(seq_count, STREAM_EXTENT, HEADS, HD).transpose(0, 2, 1, 3).reshape(seq_count * HEADS, STREAM_EXTENT, HD)

    query_heads = heads_first(query)
    key_heads = heads_first(keys)
    value_heads = heads_first(values)
    gate_heads = gate_cache.reshape(seq_count, STREAM_EXTENT, HEADS).transpose(0, 2, 1).reshape(seq_count * HEADS, STREAM_EXTENT)
    blocks = STREAM_EXTENT // TOK_DEV

    def one_block(flat):
        group = flat // blocks
        first_row = (flat % blocks) * TOK_DEV
        query_all = lax.dynamic_index_in_dim(query_heads, group, 0, False)
        key_all = lax.dynamic_index_in_dim(key_heads, group, 0, False)
        value_all = lax.dynamic_index_in_dim(value_heads, group, 0, False)
        gate_all = lax.dynamic_index_in_dim(gate_heads, group, 0, False)
        query_rows = lax.dynamic_slice_in_dim(query_all, first_row, TOK_DEV, 0)
        gate_rows = lax.dynamic_slice_in_dim(gate_all, first_row, TOK_DEV, 0)
        scores = jnp.dot(query_rows, key_all.T, preferred_element_type=jnp.float32) * (HD ** -0.5)
        scores = scores + gate_rows[:, None] - gate_all[None, :]
        row_pos = first_row + jnp.arange(TOK_DEV, dtype=jnp.int32)[:, None]
        col_pos = jnp.arange(STREAM_EXTENT, dtype=jnp.int32)[None, :]
        scores = jnp.where(col_pos <= row_pos, scores, neg_large)
        weights = jnp.exp(scores - jnp.max(scores, axis=1, keepdims=True))
        weights_low = weights.astype(jnp.bfloat16)
        summed = jnp.dot(weights_low, value_all, preferred_element_type=jnp.float32)
        return summed / jnp.sum(weights, axis=1, keepdims=True)

    outputs = lax.map(one_block, jnp.arange(seq_count * HEADS * blocks, dtype=jnp.int32))
    outputs = outputs.reshape(seq_count, HEADS, STREAM_EXTENT, HD).transpose(0, 2, 1, 3)
    return outputs.reshape(seq_count * STREAM_EXTENT, HEADS * HD).astype(jnp.bfloat16)


def reference(hidden_in, w_convb, w_convc, w_convx, w_query, w_key, w_value, conv_taps, gate_cache, w_out_conv, w_out_attn):
    hidden_in = jnp.roll(hidden_in, -ROLL_ROWS, axis=0)
    gate_cache = jnp.roll(gate_cache, -ROLL_ROWS, axis=0)
    gate_b = project(hidden_in, w_convb)
    gate_c = project(hidden_in, w_convc)
    conv_values = project(hidden_in, w_convx)
    query = project(hidden_in, w_query)
    keys = project(hidden_in, w_key)
    values = project(hidden_in, w_value)
    conv_out = short_conv(gate_b, gate_c, conv_values, conv_taps)
    attn_out = attention(query, keys, values, gate_cache)
    conv_group = CONV // N_TP
    attn_group = HEADS * HD // N_TP
    summed = jnp.zeros((hidden_in.shape[0], D), jnp.float32)
    for group in range(N_TP):
        value_partial = jnp.dot(conv_out[:, group * conv_group:(group + 1) * conv_group],
                          w_out_conv[group * conv_group:(group + 1) * conv_group],
                          preferred_element_type=jnp.float32)
        value_partial = value_partial + jnp.dot(attn_out[:, group * attn_group:(group + 1) * attn_group],
                                    w_out_attn[group * attn_group:(group + 1) * attn_group],
                                    preferred_element_type=jnp.float32)
        summed = summed + lax.optimization_barrier(value_partial.astype(jnp.bfloat16)).astype(jnp.float32)
    return jnp.roll(summed.astype(jnp.bfloat16), ROLL_ROWS, axis=0)
```

```python
import functools

import jax
import jax.numpy as jnp
from jax import lax
from jax.experimental import pallas as pl
from jax.experimental.pallas import tpu as pltpu
from jax.sharding import PartitionSpec as P

neg_large = -1e30


def passed_along(value, axis, steps):
    count = lax.axis_size(axis)
    pairs = [(source, (source + steps) % count) for source in range(count)]
    return lax.ppermute(value, axis, pairs)


def shortened(shard):

    def short(part):
        return part.astype(jnp.bfloat16) if part.dtype == jnp.float32 else part

    return jax.tree.map(short, shard)


def project(weight_rows, hidden_in):
    return jnp.dot(hidden_in, weight_rows, preferred_element_type=jnp.float32)


def absorb(attn_state, query_heads, gate_rows, key_heads, value_heads, gate_cols, allowed):
    running_max, row_total, weighted = attn_state
    score_scale = query_heads.shape[2] ** (-0.5)
    scores = (
        jnp.einsum("qhd,khd->hqk", query_heads, key_heads, preferred_element_type=jnp.float32)
        * score_scale
    )
    scores = scores + gate_rows.T[:, :, None] - gate_cols.T[:, None, :]
    if allowed is not None:
        scores = jnp.where(allowed[None], scores, neg_large)
    new_max = jnp.maximum(running_max, jnp.max(scores, axis=2))
    weights = jnp.exp(scores - new_max[:, :, None])
    factor = jnp.exp(running_max - new_max)
    row_total = row_total * factor + jnp.sum(weights, axis=2)
    weighted = weighted * factor[:, :, None] + jnp.einsum(
        "hqk,khd->hqd",
        weights.astype(jnp.bfloat16),
        value_heads,
        preferred_element_type=jnp.float32,
    )
    return (new_max, row_total, weighted)


def shards(
    hidden_in,
    w_convb,
    w_convc,
    w_convx,
    w_query,
    w_key,
    w_value,
    conv_taps,
    gate_cache,
    w_out_conv,
    w_out_attn,
):
    tok_rows = hidden_in.shape[0]
    head_count = gate_cache.shape[1]
    attn_width = w_query.shape[1]
    head_depth = attn_width // head_count
    axis_length = lax.axis_size("sp")
    group_span = axis_length // 4
    seq_index = lax.axis_index("sp")
    position = (seq_index - group_span // 2) % group_span
    pieces = (
        lax.all_gather(w_convb, "sp", axis=0, tiled=True),
        lax.all_gather(w_convc, "sp", axis=0, tiled=True),
        lax.all_gather(w_convx, "sp", axis=0, tiled=True),
        lax.all_gather(w_query, "sp", axis=0, tiled=True),
        lax.all_gather(w_key, "sp", axis=0, tiled=True),
        lax.all_gather(w_value, "sp", axis=0, tiled=True),
    )
    projected = tuple((project(weight_rows, hidden_in) for weight_rows in pieces))
    gate_b, gate_c, conv_values, query, keys, values = [
        partial_total.astype(jnp.bfloat16) for partial_total in projected
    ]
    conv_input = (gate_c.astype(jnp.float32) * conv_values.astype(jnp.float32)).astype(jnp.bfloat16)
    last_rows = conv_input[tok_rows - 2 :]
    query_heads = query.reshape(tok_rows, head_count, head_depth)
    key_heads = keys.reshape(tok_rows, head_count, head_depth)
    value_heads = values.reshape(tok_rows, head_count, head_depth)
    gate_rows = lax.dynamic_slice_in_dim(gate_cache, seq_index * tok_rows, tok_rows, 0)

    def gates_back(distance):
        source = (seq_index - distance + axis_length) % axis_length
        return lax.dynamic_slice_in_dim(gate_cache, source * tok_rows, tok_rows, 0)

    row_ids = jnp.arange(tok_rows, dtype=jnp.int32)
    allowed = row_ids[None, :] <= row_ids[:, None]
    initial = (
        jnp.full((head_count, tok_rows), neg_large, jnp.float32),
        jnp.zeros((head_count, tok_rows), jnp.float32),
        jnp.zeros((head_count, tok_rows, head_depth), jnp.float32),
    )
    attn_state = absorb(initial, query_heads, gate_rows, key_heads, value_heads, gate_rows, allowed)
    edge_rows = passed_along(last_rows, "sp", 1)
    payload = (key_heads, value_heads)
    arrived = jax.tree.map(
        lambda part, own: part.astype(own.dtype), passed_along(shortened(payload), "sp", 1), payload
    )
    travel = (arrived[0], arrived[1])
    first_gates = gates_back(1)
    attn_state = lax.cond(
        position >= 1,
        lambda current: absorb(
            current, query_heads, gate_rows, travel[0], travel[1], first_gates, None
        ),
        lambda current: current,
        attn_state,
    )

    def relay_turn(turn_index, carried):
        present_memory, moving = carried
        moving = passed_along((moving[0], moving[1]), "sp", 1)
        source_gates = gates_back(turn_index)
        present_memory = lax.cond(
            turn_index <= position,
            lambda present: absorb(
                present, query_heads, gate_rows, moving[0], moving[1], source_gates, None
            ),
            lambda present: present,
            present_memory,
        )
        return (present_memory, moving)

    attn_state, travel = lax.fori_loop(2, group_span, relay_turn, (attn_state, travel))
    edge_rows = jnp.where(position > 0, edge_rows, jnp.zeros_like(edge_rows))
    padded = lax.optimization_barrier(jnp.concatenate([edge_rows, conv_input], axis=0)).astype(
        jnp.float32
    )
    mixed_conv = (
        conv_taps[0] * padded[:tok_rows]
        + conv_taps[1] * padded[1 : tok_rows + 1]
        + conv_taps[2] * padded[2:]
    )
    conv_out = (gate_b.astype(jnp.float32) * mixed_conv).astype(jnp.bfloat16)
    running_max, row_total, weighted = attn_state
    attn_out = (
        (weighted / row_total[:, :, None])
        .transpose(1, 0, 2)
        .reshape(tok_rows, attn_width)
        .astype(jnp.bfloat16)
    )
    return lax.psum_scatter(
        (
            jnp.dot(conv_out, w_out_conv, preferred_element_type=jnp.float32)
            + jnp.dot(attn_out, w_out_attn, preferred_element_type=jnp.float32)
        ).astype(jnp.bfloat16),
        "tp",
        scatter_dimension=0,
        tiled=True,
    )


MESH = pl.DeviceIdType.MESH
N_CHUNKS = 4


def fused_kernel(
    small_ref,
    hidden_ref,
    wq_ref,
    wk_ref,
    wv_ref,
    wc_ref,
    wx_ref,
    wb_ref,
    woa_ref,
    woc_ref,
    out_ref,
    hbuf,
    wbuf,
    small,
    proj,
    woa,
    woc,
    acts,
    act_in,
    pbuf,
    rx_core,
    y_send,
    y_recv,
    s_small,
    r_small,
    s_w,
    r_w,
    s_wx,
    s_wc,
    s_hx,
    s_hz,
    s_hy,
    r_h,
    s_act,
    r_act,
    s_core,
    r_core,
    s_y,
    r_y,
    l_wo,
):
    sp = lax.axis_index("sp")
    tp = lax.axis_index("tp")
    z, x = sp // 2, sp % 2
    y, c = tp // 2, tp % 2
    rows = hidden_ref.shape[0]
    half_rows = rows // 2
    half_h = z % 2
    owner_core = z // 2

    def at(zz, xx, yy, cc):
        return {"sp": zz * 2 + xx, "tp": yy * 2 + cc}

    def remote(src, dst, ss, rs, dev):
        return pltpu.make_async_remote_copy(
            src_ref=src, dst_ref=dst, send_sem=ss, recv_sem=rs, device_id=dev, device_id_type=MESH
        )

    core_mate = at(z, x, y, 1 - c)
    x_mate = at(z, 1 - x, y, c)
    y_mate = at(z, x, 1 - y, c)

    barrier = pltpu.get_barrier_semaphore()

    @pl.loop(0, 8)
    def _(s):
        for cc in range(2):
            pl.semaphore_signal(
                barrier, inc=1, device_id={"sp": s, "tp": y * 2 + cc}, device_id_type=MESH
            )

    pl.semaphore_signal(barrier, inc=1, device_id=y_mate, device_id_type=MESH)
    pl.semaphore_wait(barrier, 17)

    root_z = (2 * c + x, (2 * c + x + 1) % 4)
    root_x = (1, 0)
    block_of = (root_z[0] * 2 + 1, root_z[1] * 2)
    seq_mine = ((sp + 7) % 8) // 2
    x_mine, c_mine = seq_mine % 2, seq_mine // 2
    my_rows = pl.ds(pl.multiple_of(y * half_rows, half_rows), half_rows)
    other_rows = pl.ds(pl.multiple_of((1 - y) * half_rows, half_rows), half_rows)

    def fan_out(i, src, go):
        for step in range(1, 4):
            zz = (z + step) % 4
            copy = remote(src, hbuf.at[i, my_rows], s_hz.at[i, step - 1], r_h.at[i, 0], at(zz, x, y, c))
            go(copy)

    def start(copy):
        copy.start()

    for i in range(2):
        is_root = z == root_z[i]

        @pl.when(is_root & (x == root_x[i]))
        def _():
            fan_out(i, hidden_ref.at[my_rows], start)
            pltpu.make_async_copy(
                hidden_ref.at[my_rows], hbuf.at[i, my_rows], r_h.at[i, 0]
            ).start()
            pltpu.make_async_copy(
                hidden_ref.at[other_rows], hbuf.at[i, other_rows], r_h.at[i, 1]
            ).start()

    def inject_copy():
        slot = 1 - x
        return remote(
            hidden_ref.at[my_rows], hbuf.at[slot, my_rows], s_hx, r_h.at[slot, 0], x_mate
        )

    injects = (c == c_mine) & (x_mine != x)

    @pl.when(injects)
    def _():
        inject_copy().start()

    sources = (wq_ref, wk_ref, wv_ref, wc_ref, wx_ref, wb_ref)

    def tile(j, s, cc):
        return wbuf.at[
            j,
            pl.ds(pl.multiple_of(s * rows, rows), rows),
            pl.ds(pl.multiple_of(cc * 128, 128), 128),
        ]

    def own_tile(j, cc, h):
        src = sources[2 * j + cc].at[:, pl.ds(h * 128, 128)]
        zt = 2 * c + h
        return zt, src, remote(
            src, tile(j, sp, cc), s_w.at[j, cc, h], r_w.at[j, sp, cc], at(zt, x, y, cc)
        )

    for j in range(3):
        for cc in range(2):
            for h in range(2):
                zt, src, copy = own_tile(j, cc, h)
                keep = (zt == z) & (c == cc)

                @pl.when(keep)
                def _():
                    pltpu.make_async_copy(src, tile(j, sp, cc), r_w.at[j, sp, cc]).start()

                @pl.when(jnp.logical_not(keep))
                def _():
                    copy.start()

    small_copy = remote(small_ref, small, s_small, r_small, core_mate)

    @pl.when(c == owner_core)
    def _():
        small_copy.start()
        pltpu.make_async_copy(small_ref, small, r_small).start()

    wo_copies = (
        pltpu.make_async_copy(woa_ref, woa, l_wo.at[0]),
        pltpu.make_async_copy(woc_ref, woc, l_wo.at[1]),
    )
    for copy in wo_copies:
        copy.start()

    def hid_y(i):
        return remote(
            hbuf.at[i, my_rows], hbuf.at[i, my_rows], s_hy.at[i], r_h.at[i, 1], y_mate
        )

    def hid_wait(i, k, part):
        remote(hbuf.at[i, part], hbuf.at[i, part], s_hy.at[i], r_h.at[i, k], y_mate).wait_recv()

    def has_local(i):
        return (z == root_z[i]) & (x == root_x[i])

    for i in range(2):

        @pl.when((z == root_z[i]) & (x != root_x[i]))
        def _():
            hid_wait(i, 0, my_rows)
            fan_out(i, hbuf.at[i, my_rows], start)
            hid_y(i).start()

    def fwd_x(j, zz):
        t = tile(j, zz * 2 + x, c)
        return remote(t, t, s_wx.at[j, zz], r_w.at[j, zz * 2 + x, c], x_mate)

    def fwd_core(j, s):
        t = tile(j, s, c)
        return remote(t, t, s_wc.at[j, s], r_w.at[j, s, c], core_mate)

    def tile_wait(j, s, cc):
        t = tile(j, s, cc)
        remote(t, t, s_wc.at[j, s], r_w.at[j, s, cc], core_mate).wait_recv()

    def line_forward(j):
        @pl.loop(0, 4)
        def _(k):
            zz = (z + k) % 4
            tile_wait(j, zz * 2 + x, c)
            fwd_x(j, zz).start()
            fwd_core(j, zz * 2 + x).start()

    def cross_forward(j):
        @pl.loop(0, 4)
        def _(k):
            zz = (z + k) % 4
            tile_wait(j, zz * 2 + 1 - x, c)
            fwd_core(j, zz * 2 + 1 - x).start()

    def mate_wait(j):
        @pl.loop(0, 8)
        def _(s):
            tile_wait(j, s, 1 - c)

    def project_pair(j):
        @pl.loop(0, 2)
        def _(i):
            proj[j, i] = jnp.dot(
                hbuf[i], wbuf[j], preferred_element_type=jnp.float32
            ).astype(jnp.bfloat16)

    line_forward(0)
    for i in range(2):

        @pl.when(z != root_z[i])
        def _():
            hid_wait(i, 0, my_rows)
            hid_y(i).start()

        @pl.when(has_local(i))
        def _():
            hid_wait(i, 0, my_rows)

    cross_forward(0)
    line_forward(1)
    cross_forward(1)
    for i in range(2):
        hid_wait(i, 1, other_rows)
    mate_wait(0)
    project_pair(0)
    mate_wait(1)
    project_pair(1)
    line_forward(2)
    cross_forward(2)

    pltpu.make_async_copy(small_ref, small, r_small).wait()

    depth = 64
    lane_head = lax.broadcasted_iota(jnp.int32, (rows, 128), 1) // depth
    gates = [
        small[:, pl.ds(pl.multiple_of(block_of[i] * rows, rows), rows)] for i in range(2)
    ]
    gates_t = [g.T for g in gates]
    causal = lax.broadcasted_iota(jnp.int32, (rows, rows), 0) >= lax.broadcasted_iota(
        jnp.int32, (rows, rows), 1
    )
    first = half_h == 0
    for i in range(2):
        q = proj[0, i, :, :128]
        merged = None
        for hh in range(2):
            col = jnp.where(first, gates_t[i][:, hh : hh + 1], gates_t[i][:, 2 + hh : 3 + hh])
            scores = []
            for k in range(i + 1):
                keys = proj[0, k, :, 128:]
                keys = jnp.where(lane_head == hh, keys, jnp.zeros_like(keys))
                row = jnp.where(first, gates[k][hh : hh + 1], gates[k][2 + hh : 3 + hh])
                s = (
                    lax.dot_general(
                        q, keys, (((1,), (1,)), ((), ())), preferred_element_type=jnp.float32
                    )
                    * depth ** (-0.5)
                    + col
                    - row
                )
                if k == i:
                    s = jnp.where(causal, s, neg_large)
                scores.append(s)
            top = jnp.max(scores[0], axis=1, keepdims=True)
            for s in scores[1:]:
                top = jnp.maximum(top, jnp.max(s, axis=1, keepdims=True))
            total, weighted = None, None
            for k, s in enumerate(scores):
                w = jnp.exp(s - top)
                t = jnp.sum(w, axis=1, keepdims=True)
                a = jnp.dot(
                    w.astype(jnp.bfloat16), proj[1, k, :, :128], preferred_element_type=jnp.float32
                )
                total = t if total is None else total + t
                weighted = a if weighted is None else weighted + a
            done = weighted / total
            merged = done if merged is None else jnp.where(lane_head == 0, merged, done)
        acts[0, i] = merged.astype(jnp.bfloat16)

    lanes_h = pl.ds(pl.multiple_of(half_h * 128, 128), 128)

    def act_copy(kind, i):
        return remote(
            acts.at[kind, i],
            act_in.at[kind, :, lanes_h],
            s_act.at[kind, i],
            r_act.at[kind, half_h],
            at(root_z[i], root_x[i], y, owner_core),
        )

    def act_stays(i):
        return has_local(i) & (c == owner_core)

    def send_acts(kind):
        for i in range(2):

            @pl.when(act_stays(i))
            def _():
                pltpu.make_async_copy(
                    acts.at[kind, i], act_in.at[kind, :, lanes_h], r_act.at[kind, half_h]
                ).start()

            @pl.when(jnp.logical_not(act_stays(i)))
            def _():
                act_copy(kind, i).start()

    def wait_acts(kind):
        for h in range(2):
            remote(
                acts.at[kind, 0],
                act_in.at[kind, :, pl.ds(h * 128, 128)],
                s_act.at[kind, 0],
                r_act.at[kind, h],
                core_mate,
            ).wait_recv()

    send_acts(0)

    mate_wait(2)
    project_pair(2)
    row_id = lax.broadcasted_iota(jnp.int32, (2 * rows, 128), 0)
    gate_c = jnp.concatenate([proj[1, 0, :, 128:], proj[1, 1, :, 128:]], axis=0)
    conv_v = jnp.concatenate([proj[2, 0, :, :128], proj[2, 1, :, :128]], axis=0)
    gate_b = jnp.concatenate([proj[2, 0, :, 128:], proj[2, 1, :, 128:]], axis=0)
    conv_in = (
        (gate_c.astype(jnp.float32) * conv_v.astype(jnp.float32))
        .astype(jnp.bfloat16)
        .astype(jnp.float32)
    )
    taps = [jnp.where(first, small[4 + k : 5 + k, :128], small[4 + k : 5 + k, 128:256]) for k in range(3)]
    mixed = taps[2] * conv_in
    for back in (1, 2):
        moved = jnp.where(row_id >= back, pltpu.roll(conv_in, back, 0), 0.0)
        mixed = mixed + taps[2 - back] * moved
    conv_out = (gate_b.astype(jnp.float32) * mixed).astype(jnp.bfloat16)
    acts[1, 0] = conv_out[:rows]
    acts[1, 1] = conv_out[rows:]
    send_acts(1)

    for copy in wo_copies:
        copy.wait()
    wait_acts(0)
    wait_acts(1)

    part_rows = pbuf.shape[2]
    width = pbuf.shape[3] // N_CHUNKS

    def cols(n):
        return pl.ds(n * width, width)

    def core_copy(n):
        return remote(
            pbuf.at[:, 1 - c, :, cols(n)],
            rx_core.at[:, :, cols(n)],
            s_core.at[n],
            r_core.at[n],
            core_mate,
        )

    def y_copy(n):
        return remote(y_send.at[:, cols(n)], y_recv.at[:, cols(n)], s_y.at[n], r_y.at[n], y_mate)

    def out_chunk(n):
        part = jnp.dot(
            act_in[0], woa[:, cols(n)], preferred_element_type=jnp.float32
        ) + jnp.dot(act_in[1], woc[:, cols(n)], preferred_element_type=jnp.float32)
        part = part.astype(jnp.bfloat16)
        for yy in range(2):
            for cc in range(2):
                first_row = (yy * 2 + cc) * part_rows
                pbuf[yy, cc, :, cols(n)] = part[first_row : first_row + part_rows]
        core_copy(n).start()

    def pass_chunk(n):
        core_copy(n).wait_recv()
        y_send[:, cols(n)] = (
            pbuf[1 - y, c, :, cols(n)].astype(jnp.float32)
            + rx_core[1 - y, :, cols(n)].astype(jnp.float32)
        ).astype(jnp.bfloat16)
        y_copy(n).start()

    for n in range(N_CHUNKS):
        out_chunk(n)
        if n >= 1:
            pass_chunk(n - 1)
    pass_chunk(N_CHUNKS - 1)
    for n in range(N_CHUNKS):
        y_copy(n).wait_recv()
        out_ref[:, cols(n)] = (
            pbuf[y, c, :, cols(n)].astype(jnp.float32)
            + rx_core[y, :, cols(n)].astype(jnp.float32)
            + y_recv[:, cols(n)].astype(jnp.float32)
        ).astype(jnp.bfloat16)

    for n in range(N_CHUNKS):
        core_copy(n).wait_send()
        y_copy(n).wait_send()
    for kind in range(2):
        for i in range(2):

            @pl.when(jnp.logical_not(act_stays(i)))
            def _():
                act_copy(kind, i).wait_send()

    @pl.when(c == owner_core)
    def _():
        small_copy.wait_send()

    @pl.when(injects)
    def _():
        inject_copy().wait_send()

    for i in range(2):

        @pl.when(z == root_z[i])
        def _():
            fan_out(i, hbuf.at[i, my_rows], lambda copy: copy.wait_send())

        @pl.when(jnp.logical_not(has_local(i)))
        def _():
            hid_y(i).wait_send()

    for j in range(3):
        for cc in range(2):
            for h in range(2):
                zt, _src, copy = own_tile(j, cc, h)

                @pl.when(jnp.logical_not((zt == z) & (c == cc)))
                def _():
                    copy.wait_send()

        @pl.loop(0, 4)
        def _(zz):
            fwd_x(j, zz).wait_send()

        @pl.loop(0, 8)
        def _(s):
            fwd_core(j, s).wait_send()


def fused_shards(
    hidden_in,
    w_convb,
    w_convc,
    w_convx,
    w_query,
    w_key,
    w_value,
    conv_taps,
    gate_cache,
    w_out_conv,
    w_out_attn,
):
    tok_rows, model = hidden_in.shape
    total_rows = gate_cache.shape[0]
    out_rows = tok_rows // 4
    small = jnp.concatenate(
        [
            gate_cache.T,
            jnp.pad(conv_taps, ((0, 1), (0, total_rows - conv_taps.shape[1]))),
        ],
        axis=0,
    )
    bf16 = jnp.bfloat16
    dma = pltpu.SemaphoreType.DMA
    any_spec = pl.BlockSpec(memory_space=pl.ANY)
    return pl.pallas_call(
        fused_kernel,
        out_shape=jax.ShapeDtypeStruct((out_rows, model), bf16),
        in_specs=[any_spec] * 10,
        out_specs=pl.BlockSpec(memory_space=pltpu.VMEM),
        scratch_shapes=[
            pltpu.VMEM((2, tok_rows, model), bf16),
            pltpu.VMEM((3, model, 256), bf16),
            pltpu.VMEM((8, total_rows), jnp.float32),
            pltpu.VMEM((3, 2, tok_rows, 256), bf16),
            pltpu.VMEM(w_out_attn.shape, bf16),
            pltpu.VMEM(w_out_conv.shape, bf16),
            pltpu.VMEM((2, 2, tok_rows, 128), bf16),
            pltpu.VMEM((2, tok_rows, 256), bf16),
            pltpu.VMEM((2, 2, out_rows, model), bf16),
            pltpu.VMEM((2, out_rows, model), bf16),
            pltpu.VMEM((out_rows, model), bf16),
            pltpu.VMEM((out_rows, model), bf16),
            dma,
            dma,
            dma((3, 2, 2)),
            dma((3, 8, 2)),
            dma((3, 4)),
            dma((3, 8)),
            dma,
            dma((2, 3)),
            dma((2,)),
            dma((2, 2)),
            dma((2, 2)),
            dma((2, 2)),
            dma((N_CHUNKS,)),
            dma((N_CHUNKS,)),
            dma((N_CHUNKS,)),
            dma((N_CHUNKS,)),
            dma((2,)),
        ],
        compiler_params=pltpu.CompilerParams(collective_id=0, has_side_effects=True),
    )(
        small,
        hidden_in,
        w_query,
        w_key,
        w_value,
        w_convc,
        w_convx,
        w_convb,
        w_out_attn,
        w_out_conv,
    )


def solution(mesh):
    one_device = shards
    if mesh.shape["sp"] // 4 == 2 and mesh.shape["tp"] == 4:
        one_device = fused_shards
    return jax.shard_map(
        one_device,
        mesh=mesh,
        in_specs=(
            P("sp", None),
            P("sp", "tp"),
            P("sp", "tp"),
            P("sp", "tp"),
            P("sp", "tp"),
            P("sp", "tp"),
            P("sp", "tp"),
            P(None, "tp"),
            P(None, "tp"),
            P("tp", None),
            P("tp", None),
        ),
        out_specs=P(("sp", "tp"), None),
        check_vma=False,
    )
```

```python
import functools

import jax
import jax.numpy as jnp
from jax import lax
from jax.experimental import pallas as pl
from jax.experimental.pallas import tpu as pltpu
from jax.sharding import PartitionSpec as P

neg_large = -1e30


def passed_along(value, axis, steps):
    count = lax.axis_size(axis)
    pairs = [(source, (source + steps) % count) for source in range(count)]
    return lax.ppermute(value, axis, pairs)


def shortened(shard):

    def short(part):
        return part.astype(jnp.bfloat16) if part.dtype == jnp.float32 else part

    return jax.tree.map(short, shard)


def project(weight_rows, hidden_in):
    return jnp.dot(hidden_in, weight_rows, preferred_element_type=jnp.float32)


def absorb(attn_state, query_heads, gate_rows, key_heads, value_heads, gate_cols, allowed):
    running_max, row_total, weighted = attn_state
    score_scale = query_heads.shape[2] ** (-0.5)
    scores = (
        jnp.einsum("qhd,khd->hqk", query_heads, key_heads, preferred_element_type=jnp.float32)
        * score_scale
    )
    scores = scores + gate_rows.T[:, :, None] - gate_cols.T[:, None, :]
    if allowed is not None:
        scores = jnp.where(allowed[None], scores, neg_large)
    new_max = jnp.maximum(running_max, jnp.max(scores, axis=2))
    weights = jnp.exp(scores - new_max[:, :, None])
    factor = jnp.exp(running_max - new_max)
    row_total = row_total * factor + jnp.sum(weights, axis=2)
    weighted = weighted * factor[:, :, None] + jnp.einsum(
        "hqk,khd->hqd",
        weights.astype(jnp.bfloat16),
        value_heads,
        preferred_element_type=jnp.float32,
    )
    return (new_max, row_total, weighted)


def shards(
    hidden_in,
    w_convb,
    w_convc,
    w_convx,
    w_query,
    w_key,
    w_value,
    conv_taps,
    gate_cache,
    w_out_conv,
    w_out_attn,
):
    tok_rows = hidden_in.shape[0]
    head_count = gate_cache.shape[1]
    attn_width = w_query.shape[1]
    head_depth = attn_width // head_count
    axis_length = lax.axis_size("sp")
    group_span = axis_length // 4
    seq_index = lax.axis_index("sp")
    position = (seq_index - group_span // 2) % group_span
    pieces = (
        lax.all_gather(w_convb, "sp", axis=0, tiled=True),
        lax.all_gather(w_convc, "sp", axis=0, tiled=True),
        lax.all_gather(w_convx, "sp", axis=0, tiled=True),
        lax.all_gather(w_query, "sp", axis=0, tiled=True),
        lax.all_gather(w_key, "sp", axis=0, tiled=True),
        lax.all_gather(w_value, "sp", axis=0, tiled=True),
    )
    projected = tuple((project(weight_rows, hidden_in) for weight_rows in pieces))
    gate_b, gate_c, conv_values, query, keys, values = [
        partial_total.astype(jnp.bfloat16) for partial_total in projected
    ]
    conv_input = (gate_c.astype(jnp.float32) * conv_values.astype(jnp.float32)).astype(jnp.bfloat16)
    last_rows = conv_input[tok_rows - 2 :]
    query_heads = query.reshape(tok_rows, head_count, head_depth)
    key_heads = keys.reshape(tok_rows, head_count, head_depth)
    value_heads = values.reshape(tok_rows, head_count, head_depth)
    gate_rows = lax.dynamic_slice_in_dim(gate_cache, seq_index * tok_rows, tok_rows, 0)

    def gates_back(distance):
        source = (seq_index - distance + axis_length) % axis_length
        return lax.dynamic_slice_in_dim(gate_cache, source * tok_rows, tok_rows, 0)

    row_ids = jnp.arange(tok_rows, dtype=jnp.int32)
    allowed = row_ids[None, :] <= row_ids[:, None]
    initial = (
        jnp.full((head_count, tok_rows), neg_large, jnp.float32),
        jnp.zeros((head_count, tok_rows), jnp.float32),
        jnp.zeros((head_count, tok_rows, head_depth), jnp.float32),
    )
    attn_state = absorb(initial, query_heads, gate_rows, key_heads, value_heads, gate_rows, allowed)
    edge_rows = passed_along(last_rows, "sp", 1)
    payload = (key_heads, value_heads)
    arrived = jax.tree.map(
        lambda part, own: part.astype(own.dtype), passed_along(shortened(payload), "sp", 1), payload
    )
    travel = (arrived[0], arrived[1])
    first_gates = gates_back(1)
    attn_state = lax.cond(
        position >= 1,
        lambda current: absorb(
            current, query_heads, gate_rows, travel[0], travel[1], first_gates, None
        ),
        lambda current: current,
        attn_state,
    )

    def relay_turn(turn_index, carried):
        present_memory, moving = carried
        moving = passed_along((moving[0], moving[1]), "sp", 1)
        source_gates = gates_back(turn_index)
        present_memory = lax.cond(
            turn_index <= position,
            lambda present: absorb(
                present, query_heads, gate_rows, moving[0], moving[1], source_gates, None
            ),
            lambda present: present,
            present_memory,
        )
        return (present_memory, moving)

    attn_state, travel = lax.fori_loop(2, group_span, relay_turn, (attn_state, travel))
    edge_rows = jnp.where(position > 0, edge_rows, jnp.zeros_like(edge_rows))
    padded = lax.optimization_barrier(jnp.concatenate([edge_rows, conv_input], axis=0)).astype(
        jnp.float32
    )
    mixed_conv = (
        conv_taps[0] * padded[:tok_rows]
        + conv_taps[1] * padded[1 : tok_rows + 1]
        + conv_taps[2] * padded[2:]
    )
    conv_out = (gate_b.astype(jnp.float32) * mixed_conv).astype(jnp.bfloat16)
    running_max, row_total, weighted = attn_state
    attn_out = (
        (weighted / row_total[:, :, None])
        .transpose(1, 0, 2)
        .reshape(tok_rows, attn_width)
        .astype(jnp.bfloat16)
    )
    return lax.psum_scatter(
        (
            jnp.dot(conv_out, w_out_conv, preferred_element_type=jnp.float32)
            + jnp.dot(attn_out, w_out_attn, preferred_element_type=jnp.float32)
        ).astype(jnp.bfloat16),
        "tp",
        scatter_dimension=0,
        tiled=True,
    )


MESH = pl.DeviceIdType.MESH
N_CHUNKS = 4
N_PIECES = 4
HID_LAG = 3
TILES_1 = 1
TILES_2 = 4


def fused_kernel(
    gate_ref,
    taps_ref,
    hidden_ref,
    wq_ref,
    wk_ref,
    wv_ref,
    wc_ref,
    wx_ref,
    wb_ref,
    woa_ref,
    woc_ref,
    out_ref,
    hbuf,
    wbuf,
    gate_in,
    taps_in,
    proj,
    woa,
    woc,
    acts,
    act_in,
    pbuf,
    rx_core,
    y_send,
    y_recv,
    s_small,
    r_small,
    s_w,
    r_w,
    s_wx,
    s_wc,
    s_hx,
    s_up,
    s_down,
    s_hy,
    r_h,
    r_hy,
    s_act,
    r_act,
    s_core,
    r_core,
    s_y,
    r_y,
    l_wo,
):
    sp = lax.axis_index("sp")
    tp = lax.axis_index("tp")
    z, x = sp // 2, sp % 2
    y, c = tp // 2, tp % 2
    rows = hidden_ref.shape[0]
    half_rows = rows // 2
    half_h = z % 2
    owner_core = z // 2

    def at(zz, xx, yy, cc):
        return {"sp": zz * 2 + xx, "tp": yy * 2 + cc}

    def remote(src, dst, ss, rs, dev):
        return pltpu.make_async_remote_copy(
            src_ref=src, dst_ref=dst, send_sem=ss, recv_sem=rs, device_id=dev, device_id_type=MESH
        )

    core_mate = at(z, x, y, 1 - c)
    x_mate = at(z, 1 - x, y, c)
    y_mate = at(z, x, 1 - y, c)

    barrier = pltpu.get_barrier_semaphore()

    @pl.loop(0, 8)
    def _(s):
        for cc in range(2):
            pl.semaphore_signal(
                barrier, inc=1, device_id={"sp": s, "tp": y * 2 + cc}, device_id_type=MESH
            )

    pl.semaphore_signal(barrier, inc=1, device_id=y_mate, device_id_type=MESH)
    with jax.named_scope("bar"):
        pl.semaphore_wait(barrier, 17)

    root_z = (2 * c + x, (2 * c + x + 1) % 4)
    root_x = (1, 0)
    block_of = (root_z[0] * 2 + 1, root_z[1] * 2)
    seq_mine = ((sp + 7) % 8) // 2
    x_mine, c_mine = seq_mine % 2, seq_mine // 2
    piece_rows = half_rows // N_PIECES

    def piece(yy, p):
        return pl.ds(pl.multiple_of(yy * half_rows + p * piece_rows, piece_rows), piece_rows)

    other_rows = pl.ds(pl.multiple_of((1 - y) * half_rows, half_rows), half_rows)
    my_rows = pl.ds(pl.multiple_of(y * half_rows, half_rows), half_rows)

    def has_local(i):
        return (z == root_z[i]) & (x == root_x[i])

    def hid_up(i, p, src):
        return remote(
            src, hbuf.at[i, piece(y, p)], s_up.at[i, p], r_h.at[i, p], at(z + 1, x, y, c)
        )

    def hid_down(i, p, src):
        return remote(
            src, hbuf.at[i, piece(y, p)], s_down.at[i, p], r_h.at[i, p], at(z - 1, x, y, c)
        )

    def hid_y(i, p):
        part = hbuf.at[i, piece(y, p)]
        return remote(part, part, s_hy.at[i, p], r_hy.at[i, p], y_mate)

    def goes_up(i):
        return (z >= root_z[i]) & (z < 3)

    def goes_down(i):
        return (z <= root_z[i]) & (z > 0)

    def inject_copy(p):
        slot = 1 - x
        return remote(
            hidden_ref.at[piece(y, p)],
            hbuf.at[slot, piece(y, p)],
            s_hx.at[p],
            r_h.at[slot, p],
            x_mate,
        )

    injects = (c == c_mine) & (x_mine != x)

    @pl.when(injects)
    def _():
        for p in range(N_PIECES):
            inject_copy(p).start()

    for i in range(2):

        @pl.when(has_local(i) & goes_up(i))
        def _():
            for p in range(N_PIECES):
                hid_up(i, p, hidden_ref.at[piece(y, p)]).start()

        @pl.when(has_local(i) & goes_down(i))
        def _():
            for p in range(N_PIECES):
                hid_down(i, p, hidden_ref.at[piece(y, p)]).start()

        @pl.when(has_local(i))
        def _():
            pltpu.make_async_copy(hidden_ref, hbuf.at[i], r_h.at[i, 0]).start()

    sources = (wq_ref, wk_ref, wv_ref, wc_ref, wx_ref, wb_ref)

    def tile(j, s, cc):
        return wbuf.at[
            j,
            pl.ds(pl.multiple_of(s * rows, rows), rows),
            pl.ds(pl.multiple_of(cc * 128, 128), 128),
        ]

    def own_tile(j, cc, h):
        src = sources[2 * j + cc].at[:, pl.ds(h * 128, 128)]
        zt = 2 * c + h
        return zt, src, remote(
            src, tile(j, sp, cc), s_w.at[j, cc, h], r_w.at[j, sp, cc], at(zt, x, y, cc)
        )

    def start_tiles(j):
        for cc in range(2):
            for h in range(2):
                zt, src, copy = own_tile(j, cc, h)
                keep = (zt == z) & (c == cc)

                @pl.when(keep)
                def _():
                    pltpu.make_async_copy(src, tile(j, sp, cc), r_w.at[j, sp, cc]).start()

                @pl.when(jnp.logical_not(keep))
                def _():
                    copy.start()

    start_tiles(0)

    small_copies = (
        remote(gate_ref, gate_in, s_small.at[0], r_small.at[0], core_mate),
        remote(taps_ref, taps_in, s_small.at[1], r_small.at[1], core_mate),
    )

    @pl.when(c == owner_core)
    def _():
        for copy in small_copies:
            copy.start()
        pltpu.make_async_copy(gate_ref, gate_in, r_small.at[0]).start()
        pltpu.make_async_copy(taps_ref, taps_in, r_small.at[1]).start()

    wo_copies = (
        pltpu.make_async_copy(woa_ref, woa, l_wo.at[0]),
        pltpu.make_async_copy(woc_ref, woc, l_wo.at[1]),
    )
    for copy in wo_copies:
        copy.start()

    def hid_pass(i, p):
        @pl.when(jnp.logical_not(has_local(i)))
        def _():
            part = hbuf.at[i, piece(y, p)]
            remote(part, part, s_hy.at[i, p], r_h.at[i, p], y_mate).wait_recv()

            @pl.when(goes_up(i))
            def _():
                hid_up(i, p, part).start()

            @pl.when(goes_down(i))
            def _():
                hid_down(i, p, part).start()

            hid_y(i, p).start()

    def hid_rest(i):
        @pl.when(has_local(i))
        def _():
            pltpu.make_async_copy(hidden_ref, hbuf.at[i], r_h.at[i, 0]).wait()

        @pl.when(jnp.logical_not(has_local(i)))
        def _():
            for p in range(N_PIECES):
                part = hbuf.at[i, piece(1 - y, p)]
                remote(part, part, s_hy.at[i, p], r_hy.at[i, p], y_mate).wait_recv()

    def fwd_x(j, zz):
        t = tile(j, zz * 2 + x, c)
        return remote(t, t, s_wx.at[j, zz], r_w.at[j, zz * 2 + x, c], x_mate)

    def fwd_core(j, s):
        t = tile(j, s, c)
        return remote(t, t, s_wc.at[j, s], r_w.at[j, s, c], core_mate)

    def tile_wait(j, s, cc):
        t = tile(j, s, cc)
        remote(t, t, s_wc.at[j, s], r_w.at[j, s, cc], core_mate).wait_recv()

    z_near = (z, (z // 2) * 2 + 1 - z % 2, 2 - z // 2, 3 * (1 - z // 2))

    def line_forward(t):
        j, zz = t // 4, z_near[t % 4]
        tile_wait(j, zz * 2 + x, c)
        fwd_x(j, zz).start()
        fwd_core(j, zz * 2 + x).start()

    def cross_forward(t):
        j, zz = t // 4, z_near[t % 4]
        tile_wait(j, zz * 2 + 1 - x, c)
        fwd_core(j, zz * 2 + 1 - x).start()

    def mate_wait(j):
        @pl.loop(0, 8)
        def _(s):
            tile_wait(j, s, 1 - c)

    def project_pair(j):
        @pl.loop(0, 2)
        def _(i):
            proj[j, i] = jnp.dot(
                hbuf[i], wbuf[j], preferred_element_type=jnp.float32
            ).astype(jnp.bfloat16)

    dist = [jnp.abs(z - root_z[i]) for i in range(2)]
    near_0 = dist[0] <= dist[1]

    def hid_turn(near, p):
        for i in range(2):

            @pl.when(near_0 if (i == 0) == near else jnp.logical_not(near_0))
            def _():
                hid_pass(i, p)

    pltpu.make_async_copy(gate_ref, gate_in, r_small.at[0]).wait()
    pltpu.make_async_copy(taps_ref, taps_in, r_small.at[1]).wait()

    depth = 64
    lane_head = lax.broadcasted_iota(jnp.int32, (rows, 128), 1) // depth
    gates = [
        gate_in[:, pl.ds(pl.multiple_of(block_of[i] * rows, rows), rows)] for i in range(2)
    ]
    gates_t = [jnp.concatenate([g, g], axis=0).T for g in gates]
    causal = lax.broadcasted_iota(jnp.int32, (rows, rows), 0) >= lax.broadcasted_iota(
        jnp.int32, (rows, rows), 1
    )
    first = half_h == 0

    def attend(i):
        q = proj[0, i, :, :128]
        merged = None
        for hh in range(2):
            col = jnp.where(first, gates_t[i][:, hh : hh + 1], gates_t[i][:, 2 + hh : 3 + hh])
            scores = []
            for k in range(i + 1):
                keys = proj[0, k, :, 128:]
                keys = jnp.where(lane_head == hh, keys, jnp.zeros_like(keys))
                row = jnp.where(first, gates[k][hh : hh + 1], gates[k][2 + hh : 3 + hh])
                s = (
                    lax.dot_general(
                        q, keys, (((1,), (1,)), ((), ())), preferred_element_type=jnp.float32
                    )
                    * depth ** (-0.5)
                    + col
                    - row
                )
                if k == i:
                    s = jnp.where(causal, s, neg_large)
                scores.append(s)
            top = jnp.max(scores[0], axis=1, keepdims=True)
            for s in scores[1:]:
                top = jnp.maximum(top, jnp.max(s, axis=1, keepdims=True))
            total, weighted = None, None
            for k, s in enumerate(scores):
                w = jnp.exp(s - top)
                t = jnp.sum(w, axis=1, keepdims=True)
                a = jnp.dot(
                    w.astype(jnp.bfloat16), proj[1, k, :, :128], preferred_element_type=jnp.float32
                )
                total = t if total is None else total + t
                weighted = a if weighted is None else weighted + a
            done = weighted / total
            merged = done if merged is None else jnp.where(lane_head == 0, merged, done)
        acts[0, i] = merged.astype(jnp.bfloat16)

    lanes_h = pl.ds(pl.multiple_of(half_h * 128, 128), 128)

    def act_copy(kind, i):
        return remote(
            acts.at[kind, i],
            act_in.at[kind, :, lanes_h],
            s_act.at[kind, i],
            r_act.at[kind, half_h],
            at(root_z[i], root_x[i], y, owner_core),
        )

    def act_stays(i):
        return has_local(i) & (c == owner_core)

    def send_acts(kind):
        for i in range(2):

            @pl.when(act_stays(i))
            def _():
                pltpu.make_async_copy(
                    acts.at[kind, i], act_in.at[kind, :, lanes_h], r_act.at[kind, half_h]
                ).start()

            @pl.when(jnp.logical_not(act_stays(i)))
            def _():
                act_copy(kind, i).start()

    def wait_acts(kind):
        for h in range(2):
            remote(
                acts.at[kind, 0],
                act_in.at[kind, :, pl.ds(h * 128, 128)],
                s_act.at[kind, 0],
                r_act.at[kind, h],
                core_mate,
            ).wait_recv()

    for t in range(12):
        with jax.named_scope(f"h{t}"):
            if t < N_PIECES:
                hid_turn(True, t)
            if HID_LAG <= t < HID_LAG + N_PIECES:
                hid_turn(False, t - HID_LAG)
        if t == TILES_1:
            start_tiles(1)
        if t == TILES_2:
            start_tiles(2)
        with jax.named_scope(f"l{t}"):
            line_forward(t)
            if t >= 1:
                cross_forward(t - 1)
        if t == 7:
            with jax.named_scope("hrest"):
                for i in range(2):
                    hid_rest(i)
            with jax.named_scope("mw0"):
                mate_wait(0)
            project_pair(0)
        if t == 8:
            with jax.named_scope("mw1"):
                mate_wait(1)
            project_pair(1)
        if t == 9:
            attend(0)
        if t == 10:
            attend(1)
            with jax.named_scope("sa0"):
                send_acts(0)
    cross_forward(11)


    with jax.named_scope("mw2"):
        mate_wait(2)
    project_pair(2)
    row_id = lax.broadcasted_iota(jnp.int32, (2 * rows, 128), 0)
    gate_c = jnp.concatenate([proj[1, 0, :, 128:], proj[1, 1, :, 128:]], axis=0)
    conv_v = jnp.concatenate([proj[2, 0, :, :128], proj[2, 1, :, :128]], axis=0)
    gate_b = jnp.concatenate([proj[2, 0, :, 128:], proj[2, 1, :, 128:]], axis=0)
    conv_in = (
        (gate_c.astype(jnp.float32) * conv_v.astype(jnp.float32))
        .astype(jnp.bfloat16)
        .astype(jnp.float32)
    )
    taps = [jnp.where(first, taps_in[k : k + 1, :128], taps_in[k : k + 1, 128:]) for k in range(3)]
    mixed = taps[2] * conv_in
    for back in (1, 2):
        moved = jnp.where(row_id >= back, pltpu.roll(conv_in, back, 0), 0.0)
        mixed = mixed + taps[2 - back] * moved
    conv_out = (gate_b.astype(jnp.float32) * mixed).astype(jnp.bfloat16)
    acts[1, 0] = conv_out[:rows]
    acts[1, 1] = conv_out[rows:]
    with jax.named_scope("sa1"):
        send_acts(1)

    for copy in wo_copies:
        copy.wait()
    with jax.named_scope("wa0"):
        wait_acts(0)
    with jax.named_scope("wa1"):
        wait_acts(1)

    part_rows = pbuf.shape[2]
    width = pbuf.shape[3] // N_CHUNKS

    def cols(n):
        return pl.ds(n * width, width)

    def core_copy(n):
        return remote(
            pbuf.at[:, 1 - c, :, cols(n)],
            rx_core.at[:, :, cols(n)],
            s_core.at[n],
            r_core.at[n],
            core_mate,
        )

    def y_copy(n):
        return remote(y_send.at[:, cols(n)], y_recv.at[:, cols(n)], s_y.at[n], r_y.at[n], y_mate)

    def out_chunk(n):
        part = jnp.dot(
            act_in[0], woa[:, cols(n)], preferred_element_type=jnp.float32
        ) + jnp.dot(act_in[1], woc[:, cols(n)], preferred_element_type=jnp.float32)
        part = part.astype(jnp.bfloat16)
        for yy in range(2):
            for cc in range(2):
                first_row = (yy * 2 + cc) * part_rows
                pbuf[yy, cc, :, cols(n)] = part[first_row : first_row + part_rows]
        core_copy(n).start()

    def pass_chunk(n):
        core_copy(n).wait_recv()
        y_send[:, cols(n)] = (
            pbuf[1 - y, c, :, cols(n)].astype(jnp.float32)
            + rx_core[1 - y, :, cols(n)].astype(jnp.float32)
        ).astype(jnp.bfloat16)
        y_copy(n).start()

    with jax.named_scope("outc"):
        for n in range(N_CHUNKS):
            out_chunk(n)
            if n >= 1:
                pass_chunk(n - 1)
    pass_chunk(N_CHUNKS - 1)
    for n in range(N_CHUNKS):
        y_copy(n).wait_recv()
        out_ref[:, cols(n)] = (
            pbuf[y, c, :, cols(n)].astype(jnp.float32)
            + rx_core[y, :, cols(n)].astype(jnp.float32)
            + y_recv[:, cols(n)].astype(jnp.float32)
        ).astype(jnp.bfloat16)

    for n in range(N_CHUNKS):
        core_copy(n).wait_send()
        y_copy(n).wait_send()
    for kind in range(2):
        for i in range(2):

            @pl.when(jnp.logical_not(act_stays(i)))
            def _():
                act_copy(kind, i).wait_send()

    @pl.when(c == owner_core)
    def _():
        for copy in small_copies:
            copy.wait_send()

    @pl.when(injects)
    def _():
        for p in range(N_PIECES):
            inject_copy(p).wait_send()

    for i in range(2):
        for p in range(N_PIECES):
            part = hbuf.at[i, piece(y, p)]

            @pl.when(goes_up(i))
            def _():
                hid_up(i, p, part).wait_send()

            @pl.when(goes_down(i))
            def _():
                hid_down(i, p, part).wait_send()

            @pl.when(jnp.logical_not(has_local(i)))
            def _():
                hid_y(i, p).wait_send()

    for j in range(3):
        for cc in range(2):
            for h in range(2):
                zt, _src, copy = own_tile(j, cc, h)

                @pl.when(jnp.logical_not((zt == z) & (c == cc)))
                def _():
                    copy.wait_send()

        @pl.loop(0, 4)
        def _(zz):
            fwd_x(j, zz).wait_send()

        @pl.loop(0, 8)
        def _(s):
            fwd_core(j, s).wait_send()


def fused_shards(
    hidden_in,
    w_convb,
    w_convc,
    w_convx,
    w_query,
    w_key,
    w_value,
    conv_taps,
    gate_cache,
    w_out_conv,
    w_out_attn,
):
    tok_rows, model = hidden_in.shape
    total_rows = gate_cache.shape[0]
    out_rows = tok_rows // 4
    bf16 = jnp.bfloat16
    dma = pltpu.SemaphoreType.DMA
    any_spec = pl.BlockSpec(memory_space=pl.ANY)
    return pl.pallas_call(
        fused_kernel,
        out_shape=jax.ShapeDtypeStruct((out_rows, model), bf16),
        in_specs=[any_spec] * 11,
        out_specs=pl.BlockSpec(memory_space=pltpu.VMEM),
        scratch_shapes=[
            pltpu.VMEM((2, tok_rows, model), bf16),
            pltpu.VMEM((3, model, 256), bf16),
            pltpu.VMEM((gate_cache.shape[1], total_rows), jnp.float32),
            pltpu.VMEM(conv_taps.shape, jnp.float32),
            pltpu.VMEM((3, 2, tok_rows, 256), bf16),
            pltpu.VMEM(w_out_attn.shape, bf16),
            pltpu.VMEM(w_out_conv.shape, bf16),
            pltpu.VMEM((2, 2, tok_rows, 128), bf16),
            pltpu.VMEM((2, tok_rows, 256), bf16),
            pltpu.VMEM((2, 2, out_rows, model), bf16),
            pltpu.VMEM((2, out_rows, model), bf16),
            pltpu.VMEM((out_rows, model), bf16),
            pltpu.VMEM((out_rows, model), bf16),
            dma((2,)),
            dma((2,)),
            dma((3, 2, 2)),
            dma((3, 8, 2)),
            dma((3, 4)),
            dma((3, 8)),
            dma((N_PIECES,)),
            dma((2, N_PIECES)),
            dma((2, N_PIECES)),
            dma((2, N_PIECES)),
            dma((2, N_PIECES)),
            dma((2, N_PIECES)),
            dma((2, 2)),
            dma((2, 2)),
            dma((N_CHUNKS,)),
            dma((N_CHUNKS,)),
            dma((N_CHUNKS,)),
            dma((N_CHUNKS,)),
            dma((2,)),
        ],
        compiler_params=pltpu.CompilerParams(collective_id=0, has_side_effects=True),
    )(
        gate_cache.T,
        conv_taps,
        hidden_in,
        w_query,
        w_key,
        w_value,
        w_convc,
        w_convx,
        w_convb,
        w_out_attn,
        w_out_conv,
    )


def solution(mesh):
    one_device = shards
    if mesh.shape["sp"] // 4 == 2 and mesh.shape["tp"] == 4:
        one_device = fused_shards
    return jax.shard_map(
        one_device,
        mesh=mesh,
        in_specs=(
            P("sp", None),
            P("sp", "tp"),
            P("sp", "tp"),
            P("sp", "tp"),
            P("sp", "tp"),
            P("sp", "tp"),
            P("sp", "tp"),
            P(None, "tp"),
            P(None, "tp"),
            P("tp", None),
            P("tp", None),
        ),
        out_specs=P(("sp", "tp"), None),
        check_vma=False,
    )
```
